32 devices in a mesh: ep: 8 (over z, y), tp: 4 (over x, core).
Axes of the slice: x: 2, y: 2, z: 4, core: 2. Of those that a mesh axis runs over, the one named last changes fastest.
Arguments:
- glu_value: bfloat16 [4096, 1024], P('ep', 'tp'), may hold values from -6 to 6
- glu_gate: bfloat16 [4096, 1024], P('ep', 'tp'), may hold values from -12 to 12
- conv_kernel: float32 [31, 1024], P(None, 'tp'), may hold values from -11.49474 to 11.49474
- ln_gain: float32 [1024], P('tp'), may hold values from 0.1 to 1.9
- out_weight: bfloat16 [1024, 2048], P('tp'), may hold values from -0.1875 to 0.1875
- moe_input: bfloat16 [2048, 2048], P('ep'), may hold values from -6 to 6
- moe_gain: float32 [2048], replicated, may hold values from 0.1 to 1.9
- gate_weight: bfloat16 [8, 2048, 3072], P('ep', None, 'tp'), may hold values from -0.125 to 0.125
- up_weight: bfloat16 [8, 2048, 3072], P('ep', None, 'tp'), may hold values from -0.125 to 0.125
- down_weight: bfloat16 [8, 3072, 2048], P('ep', 'tp'), may hold values from -0.109375 to 0.109375
- expert_ids: int32 [2048, 2], P('ep'), may hold values from 0 to 7, all different within a row; in each aligned block of 256 rows (0 to 255, 256 to 511, ...) at most 128 rows name the same one
- route_weight: float32 [2048, 2], P('ep'), may hold values from 0.2 to 1
Outputs:
- mixer_out: bfloat16 [4096, 2048], P(('ep', 'tp'))
- expert_out: bfloat16 [2048, 2048], P('ep', 'tp')
The draws below stay inside these ranges and needn't reach their ends.
Inputs may be any that keep to these rules, and one draw needn't show every extreme that they name: `expert_ids`: each row names 2 different experts. In the rows of one device no expert is named by more than 128 rows; the bound is reached at some expert in some device's rows.
All inputs are finite; a program needn't handle non-finite values.
Results may differ from the reference program's by a relative error of at most 0.012.
Values may be sent and summed in bfloat16 or wider, within the bound.
A program may use at most 64 MiB of HBM per device.

```python
import math
import jax
import jax.numpy as jnp
import numpy as np
from jax import lax

D = 2048
MIX = 1024
KERNEL = 31
FF = 3072
TOP = 2
TOKB_DEV = 256
EXPERTS = 8
CAP = 128
TOKA = 4096
TOKB = 2048
N_EP = 8
N_TP = 4


def draw_conv_kernel(key, part):
    base_key = jax.random.fold_in(key, 17)
    rough_key = jax.random.fold_in(key, 29)
    position = jnp.arange(MIX, dtype=jnp.float32) / MIX
    rough = jnp.exp(jax.random.uniform(rough_key, (MIX,), jnp.float32, math.log(0.6), math.log(1.6)))
    scale = jnp.exp(position * math.log(10.0)) * rough * KERNEL ** (-0.5)
    base = jnp.clip(jax.random.normal(base_key, (KERNEL, MIX), jnp.float32), -4.0, 4.0)
    return (base * scale[None, :]).astype(jnp.float32)


def level_of(key, shape, shards, low, high):
    def one(axis_at, shards_of):
        heights = jax.random.uniform(jax.random.fold_in(jax.random.fold_in(key, 6), axis_at), (shards_of,), jnp.float32, low / len(shards), high / len(shards))
        return jnp.repeat(jnp.exp(heights), shape[axis_at] // shards_of).reshape((-1,) + (1,) * (len(shape) - axis_at - 1))

    level = one(*shards[0])
    for cut in shards[1:]:
        level = level * one(*cut)
    return level


def shared_out(key, own, number, rows, number_of, top, reach, skew):
    ranking = jax.random.permutation(key, number_of)
    crowded, ordinary = load_shares(number_of, rows * top, reach, skew, True), load_shares(number_of, rows * top, reach, skew, False)
    places = jnp.arange(number_of)

    def named(tallies, offset_by):
        used = int((tallies > 0).sum())
        fixed = max(1, used // 4)
        moved = fixed + (places - fixed + offset_by * (used - fixed)) % max(1, number_of - fixed)
        return jnp.zeros((number_of,), jnp.int32).at[ranking[jnp.where(places < fixed, places, moved)]].set(jnp.asarray(tallies, jnp.int32))

    tallies = jnp.where(number % 4 == 0, named(crowded, number // 4), named(ordinary, number - number // 4 - 1))
    mixed = jax.random.permutation(jax.random.fold_in(own, 3), number_of)
    donor, receiver = mixed[0:number_of // 2 * 2:2], mixed[1:number_of // 2 * 2:2]
    margin = jnp.minimum(tallies[donor] - 1, reach - tallies[receiver]) // 2
    margin = jnp.where((donor == ranking[0]) | (receiver == ranking[0]) | (tallies[receiver] == 0), 0, jnp.maximum(margin, 0))
    moved = jax.random.randint(jax.random.fold_in(own, 4), (number_of // 2,), 0, 1 << 20) % (margin + 1)
    tallies = tallies.at[donor].add(-moved).at[receiver].add(moved)
    members = jnp.searchsorted(jnp.cumsum(tallies), jnp.arange(rows * top), side="right").astype(jnp.int32)
    grid = members.reshape(top, rows).T
    grid = grid[jax.random.permutation(jax.random.fold_in(own, 1), rows)]
    offset_by = jax.random.randint(jax.random.fold_in(own, 2), (rows, 1), 0, top)
    return jnp.take_along_axis(grid, (jnp.arange(top)[None, :] + offset_by) % top, axis=1)


def load_shares(number_of, total, most, skew, full):
    portions = [(1 << 20) // math.isqrt(rank ** skew) + 1 for rank in range(1, number_of + 1)]
    largest = most if full else min(most, max(-(-total // number_of), total * portions[0] // sum(portions)))
    least = 1 if total - largest >= number_of - 1 else 0
    counts, rest = [largest] + [least] * (number_of - 1), total - largest - least * (number_of - 1)
    while rest > 0:
        movable = [i for i in range(1, number_of) if counts[i] < largest] or [i for i in range(1, number_of) if counts[i] < most]
        pool, budget = sum([portions[i] for i in movable]), rest
        for i in movable:
            extra = min(most - counts[i], max(1, budget * portions[i] // pool), rest)
            counts[i] = counts[i] + extra
            rest = rest - extra
    return np.array(counts)


def normal_values(key, shape, scale, limit, pieces=(), kind=jnp.bfloat16):
    entries = scale * jax.random.normal(key, shape, jnp.float32)
    if pieces:
        entries = entries * level_of(key, shape, pieces, -0.22, 0.18)
    return jnp.clip(entries, -limit, limit).astype(kind)


def setup_inputs(seed: int = 0) -> dict:
    streams_of = jax.random.split(jax.random.key(seed), 13)
    glu_value = normal_values(streams_of[0], (TOKA, MIX), 1.0, 6.0, ((0, 8), (1, 4)))
    glu_gate = normal_values(streams_of[1], (TOKA, MIX), 2.0, 12.0, ((0, 8), (1, 4)))
    conv_kernel = draw_conv_kernel(jax.random.fold_in(streams_of[12], 71), 0)
    ln_gain = jnp.clip(1.0 + 0.18 * jax.random.normal(streams_of[3], (MIX,), jnp.float32), 0.1, 1.9)
    out_weight = normal_values(streams_of[4], (MIX, D), MIX ** -0.5, 0.1875, ((0, 4),))
    moe_input = normal_values(streams_of[5], (TOKB, D), 1.0, 6.0, ((0, 8),))
    moe_gain = jnp.clip(1.0 + 0.18 * jax.random.normal(streams_of[6], (D,), jnp.float32), 0.1, 1.9)
    gate_weight = normal_values(streams_of[7], (EXPERTS, D, FF), D ** -0.5, 0.125, ((0, 8), (2, 4)))
    up_weight = normal_values(streams_of[8], (EXPERTS, D, FF), D ** -0.5, 0.125, ((0, 8), (2, 4)))
    down_weight = normal_values(streams_of[9], (EXPERTS, FF, D), FF ** -0.5, 0.109375, ((0, 8), (1, 4)))
    expert_ids_keys = jax.random.split(jax.random.fold_in(streams_of[10], 1), TOKB // TOKB_DEV)
    expert_ids_turns = jax.random.permutation(jax.random.fold_in(streams_of[10], 3), TOKB // TOKB_DEV)
    expert_ids = jax.vmap(lambda own, number: shared_out(jax.random.fold_in(streams_of[10], 2), own, number, TOKB_DEV, EXPERTS, TOP, CAP, 1))(expert_ids_keys, expert_ids_turns).reshape((TOKB, TOP))
    route_weight = jnp.clip(0.2 + 0.8 * jax.random.uniform(streams_of[11], (TOKB, TOP), jnp.float32) ** level_of(streams_of[11], (TOKB, TOP), ((0, 8),), -0.2, 0.2), 0.2, 1.0)
    return {"glu_value": glu_value, "glu_gate": glu_gate, "conv_kernel": conv_kernel, "ln_gain": ln_gain, "out_weight": out_weight, "moe_input": moe_input, "moe_gain": moe_gain, "gate_weight": gate_weight, "up_weight": up_weight, "down_weight": down_weight, "expert_ids": expert_ids, "route_weight": route_weight}


eps_rms = 1e-06
eps_norm = 1e-05

def slot_numbers(expert_ids, experts, capacity):
    chosen = expert_ids.reshape(-1)
    onehot = (chosen[:, None] == jnp.arange(experts, dtype=jnp.int32)[None, :]).astype(jnp.int32)
    earlier = jnp.cumsum(onehot, axis=0) - onehot
    position = lax.optimization_barrier(jnp.sum(earlier * onehot, axis=1))
    return (chosen * capacity + position).astype(jnp.int32)

def fill_slots(normed, slot_index, experts, capacity, chosen_per_token):
    owners = jnp.full((experts * capacity,), -1, jnp.int32)
    token_of = (jnp.arange(slot_index.shape[0], dtype=jnp.int32) // chosen_per_token).astype(jnp.int32)
    owners = owners.at[slot_index].set(token_of)
    picked = jnp.take(normed, jnp.maximum(owners, 0), axis=0)
    filled = jnp.where((owners >= 0)[:, None], picked, jnp.zeros_like(picked))
    return filled.reshape(experts, capacity, normed.shape[1])

def mixer_half(glu_value, glu_gate, conv_kernel, ln_gain, out_weight):
    gated = (glu_value.astype(jnp.float32) * jax.nn.sigmoid(glu_gate.astype(jnp.float32))).astype(jnp.bfloat16)
    length = gated.shape[0]
    padded = jnp.concatenate([jnp.zeros((KERNEL - 1, MIX), jnp.bfloat16), gated], axis=0).astype(jnp.float32)
    convolved = jnp.zeros((length, MIX), jnp.float32)
    for tap_index in range(KERNEL):
        begin = KERNEL - 1 - tap_index
        convolved = convolved + conv_kernel[tap_index] * padded[begin:begin + length]
    total = lax.optimization_barrier(jnp.sum(convolved, axis=1))
    squares = lax.optimization_barrier(jnp.sum(convolved * convolved, axis=1))
    mean = total / MIX
    variance = squares / MIX - mean * mean
    scaled = (convolved - mean[:, None]) * lax.rsqrt(variance + eps_norm)[:, None] * ln_gain
    activated = jax.nn.silu(scaled).astype(jnp.bfloat16)
    group = MIX // N_TP
    result = jnp.zeros((length, D), jnp.float32)
    for part_index in range(N_TP):
        partial_sum = jnp.dot(activated[:, part_index * group:(part_index + 1) * group], out_weight[part_index * group:(part_index + 1) * group], preferred_element_type=jnp.float32).astype(jnp.bfloat16)
        result = result + partial_sum.astype(jnp.float32)
    return result.astype(jnp.bfloat16)

def run_expert(operands):
    arrived, w_gate, w_up, w_down = operands
    gate_act = jnp.dot(arrived, w_gate, preferred_element_type=jnp.float32)
    up_act = jnp.dot(arrived, w_up, preferred_element_type=jnp.float32)
    hidden = (jax.nn.silu(gate_act) * up_act).astype(jnp.bfloat16)
    group = FF // N_TP
    total = jnp.zeros((arrived.shape[0], D), jnp.float32)
    for part_index in range(N_TP):
        partial_sum = jnp.dot(hidden[:, part_index * group:(part_index + 1) * group], w_down[part_index * group:(part_index + 1) * group], preferred_element_type=jnp.float32).astype(jnp.bfloat16)
        total = total + partial_sum.astype(jnp.float32)
    return total.astype(jnp.bfloat16)

def expert_half(moe_input, moe_gain, gate_weight, up_weight, down_weight, expert_ids, route_weight):
    values = moe_input.astype(jnp.float32)
    normed = (values * lax.rsqrt(lax.optimization_barrier(jnp.mean(values * values, axis=1, keepdims=True)) + eps_rms) * moe_gain).astype(jnp.bfloat16)
    normed_blocks = normed.reshape(N_EP, TOKB_DEV, D)
    id_blocks = expert_ids.reshape(N_EP, TOKB_DEV, TOP)
    slot_index = jax.vmap(lambda ids: slot_numbers(ids, EXPERTS, CAP))(id_blocks)
    sent = jax.vmap(lambda block, slots: fill_slots(block, slots, EXPERTS, CAP, TOP))(normed_blocks, slot_index)
    by_expert = jnp.swapaxes(sent, 0, 1).reshape(EXPERTS, N_EP * CAP, D)
    answers = lax.map(run_expert, (by_expert, gate_weight, up_weight, down_weight))
    answers = jnp.swapaxes(answers.reshape(EXPERTS, N_EP, CAP, D), 0, 1).reshape(N_EP, EXPERTS * CAP, D)

    def combine(block_answers, slots, weights):
        picked = jnp.take(block_answers, slots, axis=0).astype(jnp.float32).reshape(TOKB_DEV, TOP, D)
        return lax.optimization_barrier(jnp.sum(picked * weights[:, :, None], axis=1))
    mixed = jax.vmap(combine)(answers, slot_index, route_weight.reshape(N_EP, TOKB_DEV, TOP))
    return mixed.reshape(N_EP * TOKB_DEV, D).astype(jnp.bfloat16)

def reference(glu_value, glu_gate, conv_kernel, ln_gain, out_weight, moe_input, moe_gain, gate_weight, up_weight, down_weight, expert_ids, route_weight):
    mixer_out = mixer_half(glu_value, glu_gate, conv_kernel, ln_gain, out_weight)
    expert_out = expert_half(moe_input, moe_gain, gate_weight, up_weight, down_weight, expert_ids, route_weight)
    return (mixer_out, expert_out)
```

```python
import functools

import jax
import jax.numpy as jnp
from jax import lax
from jax.experimental import pallas as pl
from jax.experimental.pallas import tpu as pltpu
from jax.sharding import PartitionSpec as P

eps_rms = 1e-06
eps_norm = 1e-05
MESH = pl.DeviceIdType.MESH
f32 = jnp.float32
bf16 = jnp.bfloat16


def kernel(
    n,
    tp,
    cap,
    group,
    reach,
    moe_ref,
    moe_gain_ref,
    ids_ref,
    ids_t_ref,
    route_ref,
    taps_ref,
    ln_gain_ref,
    value_hbm,
    gate_hbm,
    w_out_hbm,
    w_gate_hbm,
    w_up_hbm,
    w_down_hbm,
    mixer_ref,
    expert_ref,
    value,
    gate,
    w_out,
    w_gate,
    w_up,
    w_down,
    load_sem,
    slots,
    onehots,
    arrived,
    a2a_send,
    a2a_recv,
    fx_send,
    fx_recv,
    fp_send,
    fp_recv,
    fq_send,
    fq_recv,
    gated,
    halo_in,
    halo_send,
    halo_recv,
    padded,
    conv,
    stat_out,
    stat_in,
    stat_send,
    stat_recv,
    act,
    mix_out,
    mix_own,
    mix_in,
    mix_send,
    mix_recv,
    mix_x_out,
    mix_x_in,
    mix_x_send,
    mix_x_recv,
    rs_out,
    rs_own,
    rs_in,
    rs_send,
    rs_recv,
    rx_out,
    rx_in,
    rx_send,
    rx_recv,
    answer,
    returned,
    ret_send,
    ret_recv,
    total,
):
    me = lax.axis_index("ep")
    mine = lax.axis_index("tp")
    core = lax.rem(mine, 2)
    chip = mine // 2
    partner = chip * 2 + 1 - core
    chips = tp // 2
    groups = n // group
    rows = group * cap
    tokens, width = moe_ref.shape
    quarter = width // tp
    length, chan = value.shape
    halo = halo_in.shape[0]
    own_rows = length // tp

    def across(j):
        there = lax.rem(chip + j, chips)
        here = lax.rem(chip + chips - j, chips)
        return there * 2 + core, here * 2 + core

    barrier = pltpu.get_barrier_semaphore()

    def greet_ep(k, _):
        pl.semaphore_signal(
            barrier, inc=1, device_id={"ep": lax.rem(me + k, n)}, device_id_type=MESH
        )
        return 0

    lax.fori_loop(1, n, greet_ep, 0)
    for j in range(1, tp):
        pl.semaphore_signal(
            barrier, inc=1, device_id={"tp": lax.rem(mine + j, tp)}, device_id_type=MESH
        )

    loads = [
        pltpu.make_async_copy(src, dst, load_sem.at[i])
        for i, (src, dst) in enumerate(
            [
                (value_hbm, value),
                (gate_hbm, gate),
                (w_out_hbm, w_out),
                (w_gate_hbm.at[0], w_gate),
                (w_up_hbm.at[0], w_up),
                (w_down_hbm.at[0], w_down),
            ]
        )
    ]
    for load in loads:
        load.start()

    own_columns = pl.ds(pl.multiple_of(mine * quarter, 128), quarter)
    everything = moe_ref[...].astype(f32)
    inverse = lax.rsqrt(jnp.sum(everything * everything, axis=1, keepdims=True) / width + eps_rms)
    normed = (moe_ref[:, own_columns].astype(f32) * inverse * moe_gain_ref[:, own_columns]).astype(
        bf16
    )
    row = lax.broadcasted_iota(jnp.int32, (tokens, tokens), 0)
    col = lax.broadcasted_iota(jnp.int32, (tokens, tokens), 1)
    below = (col < row).astype(f32).astype(bf16)
    above = (row < col).astype(f32).astype(bf16)

    def a2a_copy(k):
        return pltpu.make_async_remote_copy(
            src_ref=slots.at[pl.ds(pl.multiple_of(k * cap, cap), cap)],
            dst_ref=arrived.at[mine, pl.ds(pl.multiple_of(k * cap, cap), cap)],
            send_sem=a2a_send.at[k],
            recv_sem=a2a_recv.at[k],
            device_id={"ep": lax.rem(me + k, n)},
            device_id_type=MESH,
        )

    def slot_rows(k):
        expert = lax.rem(me + k, n)
        member = jnp.maximum(
            (ids_t_ref[0:1, :] == expert).astype(f32), (ids_t_ref[1:2, :] == expert).astype(f32)
        )
        member = jnp.broadcast_to(member, (cap, tokens))
        place = jnp.dot(member.astype(bf16), above, preferred_element_type=f32)
        slot = lax.broadcasted_iota(jnp.int32, (cap, tokens), 0).astype(f32)
        pick = jnp.where(place == slot, member, 0.0).astype(bf16)
        return jnp.dot(pick, normed, preferred_element_type=f32).astype(bf16)

    own_slots = slot_rows(0)
    arrived[mine, 0:cap, :] = own_slots
    pl.semaphore_wait(barrier, n - 1 + tp - 1)

    def dispatch(k, _):
        slots[pl.ds(pl.multiple_of(k * cap, cap), cap), :] = slot_rows(k)
        a2a_copy(k).start()
        return 0

    lax.fori_loop(1, n, dispatch, 0)

    loads[0].wait()
    loads[1].wait()
    gated_now = (value[...].astype(f32) * jax.nn.sigmoid(gate[...].astype(f32))).astype(bf16)
    gated[...] = gated_now
    halo_copy = pltpu.make_async_remote_copy(
        src_ref=gated.at[pl.ds(length - halo, halo)],
        dst_ref=halo_in,
        send_sem=halo_send,
        recv_sem=halo_recv,
        device_id={"ep": lax.rem(me + 1, n)},
        device_id_type=MESH,
    )
    halo_copy.start()
    padded[pl.ds(halo, length), :] = gated_now.astype(f32)

    def place_of(k, _):
        expert = lax.rem(me + k, n)
        member = jnp.maximum(
            (ids_ref[:, 0:1] == expert).astype(f32), (ids_ref[:, 1:2] == expert).astype(f32)
        )
        member = jnp.broadcast_to(member, (tokens, cap))
        place = jnp.dot(below, member.astype(bf16), preferred_element_type=f32)
        slot = lax.broadcasted_iota(jnp.int32, (tokens, cap), 1).astype(f32)
        onehots[k] = jnp.where(place == slot, member, 0.0).astype(bf16)
        return 0

    lax.fori_loop(0, n, place_of, 0)

    def piece(ref, part, g):
        return ref.at[part, pl.ds(pl.multiple_of(g * rows, rows), rows)]

    def fx_copy(g, j):
        to, _ = across(j)
        return pltpu.make_async_remote_copy(
            src_ref=piece(arrived, mine, g),
            dst_ref=piece(arrived, mine, g),
            send_sem=fx_send.at[g, j - 1],
            recv_sem=fx_recv.at[g, j - 1],
            device_id={"tp": to},
            device_id_type=MESH,
        )

    def fp_copy(g):
        return pltpu.make_async_remote_copy(
            src_ref=piece(arrived, mine, g),
            dst_ref=piece(arrived, mine, g),
            send_sem=fp_send.at[g],
            recv_sem=fp_recv.at[g],
            device_id={"tp": partner},
            device_id_type=MESH,
        )

    def fq_copy(g, j):
        _, origin = across(j)
        return pltpu.make_async_remote_copy(
            src_ref=piece(arrived, origin, g),
            dst_ref=piece(arrived, origin, g),
            send_sem=fq_send.at[g, j - 1],
            recv_sem=fq_recv.at[g, j - 1],
            device_id={"tp": partner},
            device_id_type=MESH,
        )

    def forward_first(g):
        def arrival(k, _):
            @pl.when(k > 0)
            def _():
                a2a_copy(k).wait_recv()

            return 0

        lax.fori_loop(g * group, (g + 1) * group, arrival, 0)
        for j in range(1, chips):
            fx_copy(g, j).start()
        fp_copy(g).start()

    def forward_second(g):
        for j in range(1, chips):
            fx_copy(g, j).wait_recv()
            fq_copy(g, j).start()

    forward_first(0)

    halo_copy.wait_recv()
    padded[pl.ds(0, halo), :] = jnp.where(me == 0, 0.0, halo_in[...].astype(f32))
    step_rows = 64
    window = step_rows + halo

    for lane in range(0, chan, 128):

        def conv_step(i, _):
            base = pl.multiple_of(i * step_rows, step_rows)
            rows_in = padded[pl.ds(base, window), lane : lane + 128]
            result = jnp.zeros((step_rows, 128), f32)
            for shift in range(8):
                turned = rows_in if shift == 0 else pltpu.roll(rows_in, window - shift, 0)
                for tap in range(reach):
                    offset = halo - tap
                    if offset % 8 == shift:
                        begin = offset - shift
                        result = (
                            result
                            + taps_ref[tap : tap + 1, lane : lane + 128]
                            * turned[begin : begin + step_rows]
                        )
            conv[pl.ds(base, step_rows), lane : lane + 128] = result
            return 0

        lax.fori_loop(0, length // step_rows, conv_step, 0)

    convolved = conv[...]
    sums = jnp.sum(convolved, axis=1, keepdims=True)
    squares = jnp.sum(convolved * convolved, axis=1, keepdims=True)
    lanes = lax.broadcasted_iota(jnp.int32, (length, 128), 1)
    packed = jnp.where(lanes == 0, sums, jnp.where(lanes == 1, squares, 0.0))
    stat_out[...] = jnp.transpose(packed)[0:8]

    def stat_copy(j):
        return pltpu.make_async_remote_copy(
            src_ref=stat_out,
            dst_ref=stat_in.at[j - 1],
            send_sem=stat_send.at[j - 1],
            recv_sem=stat_recv.at[j - 1],
            device_id={"tp": lax.rem(mine + j, tp)},
            device_id_type=MESH,
        )

    for j in range(1, tp):
        stat_copy(j).start()

    if groups > 1:
        forward_first(1)
    forward_second(0)

    stats = stat_out[...]
    for j in range(1, tp):
        stat_copy(j).wait_recv()
        stats = stats + stat_in[j - 1]
    stats = jnp.concatenate([stats, jnp.zeros((120, length), f32)], axis=0)
    columns = jnp.transpose(stats)
    mean = columns[:, 0:1] / (chan * tp)
    variance = columns[:, 1:2] / (chan * tp) - mean * mean
    scaled = (conv[...] - mean) * lax.rsqrt(variance + eps_norm) * ln_gain_ref[...]
    act[...] = jax.nn.silu(scaled).astype(bf16)

    def mix_copy(xx):
        return pltpu.make_async_remote_copy(
            src_ref=mix_out.at[xx],
            dst_ref=mix_in.at[xx],
            send_sem=mix_send.at[xx],
            recv_sem=mix_recv.at[xx],
            device_id={"tp": partner},
            device_id_type=MESH,
        )

    def mix_part(owner):
        begin = pl.multiple_of(owner * own_rows, own_rows)
        return jnp.dot(act[pl.ds(begin, own_rows), :], w_out[...], preferred_element_type=f32)

    loads[2].wait()

    def mix_first(xx, _):
        mix_out[xx] = mix_part(xx * 2 + 1 - core).astype(bf16)
        mix_copy(xx).start()
        return 0

    def mix_second(xx, _):
        mix_own[xx] = mix_part(xx * 2 + core).astype(bf16)
        return 0

    lax.fori_loop(0, chips, mix_first, 0)
    lax.fori_loop(0, chips, mix_second, 0)

    def mix_x_copy(j):
        to, _ = across(j)
        return pltpu.make_async_remote_copy(
            src_ref=mix_x_out.at[j - 1],
            dst_ref=mix_x_in.at[j - 1],
            send_sem=mix_x_send.at[j - 1],
            recv_sem=mix_x_recv.at[j - 1],
            device_id={"tp": to},
            device_id_type=MESH,
        )

    def mix_stage():
        for xx in range(chips):
            mix_copy(xx).wait_recv()
        for j in range(1, chips):
            there = lax.rem(chip + j, chips)
            mix_x_out[j - 1] = (mix_own[there].astype(f32) + mix_in[there].astype(f32)).astype(
                bf16
            )
            mix_x_copy(j).start()

    loads[3].wait()
    loads[4].wait()
    loads[5].wait()

    def rs_copy(g, xx):
        return pltpu.make_async_remote_copy(
            src_ref=rs_out.at[g, xx],
            dst_ref=rs_in.at[g, xx],
            send_sem=rs_send.at[g, xx],
            recv_sem=rs_recv.at[g, xx],
            device_id={"tp": partner},
            device_id_type=MESH,
        )

    def rx_copy(g, j):
        to, _ = across(j)
        return pltpu.make_async_remote_copy(
            src_ref=rx_out.at[g, j - 1],
            dst_ref=rx_in.at[g, j - 1],
            send_sem=rx_send.at[g, j - 1],
            recv_sem=rx_recv.at[g, j - 1],
            device_id={"tp": to},
            device_id_type=MESH,
        )

    def ret_copy(k):
        return pltpu.make_async_remote_copy(
            src_ref=answer.at[pl.ds(pl.multiple_of(k * cap, cap), cap)],
            dst_ref=returned.at[pl.ds(pl.multiple_of(k * cap, cap), cap)],
            send_sem=ret_send.at[k],
            recv_sem=ret_recv.at[k],
            device_id={"ep": lax.rem(me + n - k, n)},
            device_id_type=MESH,
        )

    def expert_step(g):
        fp_copy(g).wait_recv()
        for j in range(1, chips):
            fq_copy(g, j).wait_recv()
        gate_act = jnp.zeros((rows, w_gate.shape[1]), f32)
        up_act = jnp.zeros((rows, w_up.shape[1]), f32)
        block = pl.ds(pl.multiple_of(g * rows, rows), rows)
        x = jnp.concatenate([arrived[part, block] for part in range(tp)], axis=1)
        gate_act = jnp.dot(x, w_gate[...], preferred_element_type=f32)
        up_act = jnp.dot(x, w_up[...], preferred_element_type=f32)
        hidden = (jax.nn.silu(gate_act) * up_act).astype(bf16)
        for xx in range(chips):
            begin = pl.multiple_of((xx * 2 + 1 - core) * quarter, 128)
            rs_out[g, xx] = jnp.dot(
                hidden, w_down[:, pl.ds(begin, quarter)], preferred_element_type=f32
            ).astype(bf16)
            rs_copy(g, xx).start()
        for xx in range(chips):
            begin = pl.multiple_of((xx * 2 + core) * quarter, 128)
            rs_own[g, xx] = jnp.dot(
                hidden, w_down[:, pl.ds(begin, quarter)], preferred_element_type=f32
            ).astype(bf16)

    def sum_step(g):
        for xx in range(chips):
            rs_copy(g, xx).wait_recv()
        for j in range(1, chips):
            there = lax.rem(chip + j, chips)
            rx_out[g, j - 1] = (rs_own[g, there].astype(f32) + rs_in[g, there].astype(f32)).astype(
                bf16
            )
            rx_copy(g, j).start()

    def return_step(g):
        result = rs_own[g, chip].astype(f32) + rs_in[g, chip].astype(f32)
        for j in range(1, chips):
            rx_copy(g, j).wait_recv()
            result = result + rx_in[g, j - 1].astype(f32)
        result = result.astype(bf16)
        answer[pl.ds(pl.multiple_of(g * rows, rows), rows), :] = result

        @pl.when(g == 0)
        def _():
            returned[0:cap, :] = result[0:cap]

        def give(k, _):
            @pl.when(k > 0)
            def _():
                ret_copy(k).start()

            return 0

        lax.fori_loop(g * group, (g + 1) * group, give, 0)

    total[...] = jnp.zeros_like(total)

    def combine_step(g):
        def take(k, _):
            @pl.when(k > 0)
            def _():
                ret_copy(k).wait_recv()

            expert = lax.rem(me + k, n)
            weight = jnp.where(ids_ref[:, 0:1] == expert, route_ref[:, 0:1], 0.0) + jnp.where(
                ids_ref[:, 1:2] == expert, route_ref[:, 1:2], 0.0
            )
            answers = returned[pl.ds(pl.multiple_of(k * cap, cap), cap), :]
            total[...] += weight * jnp.dot(onehots[k], answers, preferred_element_type=f32)
            return 0

        lax.fori_loop(g * group, (g + 1) * group, take, 0)

    def step(g, _):
        @pl.when(g + 2 < groups)
        def _():
            forward_first(g + 2)

        @pl.when(g + 1 < groups)
        def _():
            forward_second(g + 1)

        @pl.when(g < groups)
        def _():
            expert_step(g)

        @pl.when(g == 0)
        def _():
            mix_stage()

        @pl.when((g >= 1) & (g < groups + 1))
        def _():
            sum_step(g - 1)

        @pl.when((g >= 2) & (g < groups + 2))
        def _():
            return_step(g - 2)

        @pl.when(g >= 3)
        def _():
            combine_step(g - 3)

        return 0

    lax.fori_loop(0, groups + 3, step, 0)
    expert_ref[...] = total[...].astype(bf16)

    mixed = mix_own[chip].astype(f32) + mix_in[chip].astype(f32)
    for j in range(1, chips):
        mix_x_copy(j).wait_recv()
        mixed = mixed + mix_x_in[j - 1].astype(f32)
    mixer_ref[...] = mixed.astype(bf16)

    def left(k, _):
        a2a_copy(k).wait_send()
        ret_copy(k).wait_send()
        return 0

    lax.fori_loop(1, n, left, 0)
    halo_copy.wait_send()
    for j in range(1, tp):
        stat_copy(j).wait_send()
    for xx in range(chips):
        mix_copy(xx).wait_send()
    for j in range(1, chips):
        mix_x_copy(j).wait_send()

    def left_group(g, _):
        fp_copy(g).wait_send()
        for j in range(1, chips):
            fx_copy(g, j).wait_send()
            fq_copy(g, j).wait_send()
            rx_copy(g, j).wait_send()
        for xx in range(chips):
            rs_copy(g, xx).wait_send()
        return 0

    lax.fori_loop(0, groups, left_group, 0)


def on_device(
    glu_value,
    glu_gate,
    conv_kernel,
    ln_gain,
    out_weight,
    moe_input,
    moe_gain,
    gate_weight,
    up_weight,
    down_weight,
    expert_ids,
    route_weight,
):
    n = lax.axis_size("ep")
    tp = lax.axis_size("tp")
    chips = tp // 2
    length, chan = glu_value.shape
    reach = conv_kernel.shape[0]
    halo = -(-(reach - 1) // 16) * 16
    tokens, width = moe_input.shape
    hidden = gate_weight.shape[2]
    cap = 4 * max(1, tokens // n)
    group = max(1, min(n, 256 // cap))
    groups = n // group
    rows = group * cap
    quarter = width // tp
    own_rows = length // tp
    vmem = pl.BlockSpec(memory_space=pltpu.VMEM)
    hbm = pl.BlockSpec(memory_space=pl.ANY)
    dma = pltpu.SemaphoreType.DMA
    V = pltpu.VMEM
    others = max(1, chips - 1)
    return pl.pallas_call(
        functools.partial(kernel, n, tp, cap, group, reach),
        out_shape=(
            jax.ShapeDtypeStruct((own_rows, out_weight.shape[1]), bf16),
            jax.ShapeDtypeStruct((tokens, quarter), bf16),
        ),
        in_specs=[vmem] * 7 + [hbm] * 6,
        out_specs=(vmem, vmem),
        scratch_shapes=[
            V((length, chan), bf16),
            V((length, chan), bf16),
            V(out_weight.shape, bf16),
            V((width, hidden), bf16),
            V((width, hidden), bf16),
            V((hidden, width), bf16),
            dma((6,)),
            V((n * cap, quarter), bf16),
            V((n, tokens, cap), bf16),
            V((tp, n * cap, quarter), bf16),
            dma((n,)),
            dma((n,)),
            dma((groups, others)),
            dma((groups, others)),
            dma((groups,)),
            dma((groups,)),
            dma((groups, others)),
            dma((groups, others)),
            V((length, chan), bf16),
            V((halo, chan), bf16),
            dma,
            dma,
            V((length + halo, chan), f32),
            V((length, chan), f32),
            V((8, length), f32),
            V((tp - 1, 8, length), f32),
            dma((tp - 1,)),
            dma((tp - 1,)),
            V((length, chan), bf16),
            V((chips, own_rows, out_weight.shape[1]), bf16),
            V((chips, own_rows, out_weight.shape[1]), bf16),
            V((chips, own_rows, out_weight.shape[1]), bf16),
            dma((chips,)),
            dma((chips,)),
            V((others, own_rows, out_weight.shape[1]), bf16),
            V((others, own_rows, out_weight.shape[1]), bf16),
            dma((others,)),
            dma((others,)),
            V((groups, chips, rows, quarter), bf16),
            V((groups, chips, rows, quarter), bf16),
            V((groups, chips, rows, quarter), bf16),
            dma((groups, chips)),
            dma((groups, chips)),
            V((groups, others, rows, quarter), bf16),
            V((groups, others, rows, quarter), bf16),
            dma((groups, others)),
            dma((groups, others)),
            V((n * cap, quarter), bf16),
            V((n * cap, quarter), bf16),
            dma((n,)),
            dma((n,)),
            V((tokens, quarter), f32),
        ],
        compiler_params=pltpu.CompilerParams(
            collective_id=0, has_side_effects=True, vmem_limit_bytes=60 * 1024 * 1024
        ),
        name="block",
    )(
        moe_input,
        moe_gain.reshape(1, -1),
        expert_ids,
        expert_ids.T,
        route_weight,
        conv_kernel,
        ln_gain.reshape(1, -1),
        glu_value,
        glu_gate,
        out_weight,
        gate_weight,
        up_weight,
        down_weight,
    )


def solution(mesh):
    in_specs = (
        P("ep", "tp"),
        P("ep", "tp"),
        P(None, "tp"),
        P("tp"),
        P("tp", None),
        P("ep", None),
        P(),
        P("ep", None, "tp"),
        P("ep", None, "tp"),
        P("ep", "tp", None),
        P("ep", None),
        P("ep", None),
    )
    out_specs = (P(("ep", "tp"), None), P("ep", "tp"))
    return jax.shard_map(
        on_device, mesh=mesh, in_specs=in_specs, out_specs=out_specs, check_vma=False
    )
```

```python
import functools

import jax
import jax.numpy as jnp
from jax import lax
from jax.experimental import pallas as pl
from jax.experimental.pallas import tpu as pltpu
from jax.sharding import PartitionSpec as P

eps_rms = 1e-06
eps_norm = 1e-05
MESH = pl.DeviceIdType.MESH
f32 = jnp.float32
bf16 = jnp.bfloat16


def kernel(
    n,
    tp,
    cap,
    group,
    reach,
    moe_ref,
    moe_gain_ref,
    ids_ref,
    ids_t_ref,
    route_ref,
    taps_ref,
    ln_gain_ref,
    value_hbm,
    gate_hbm,
    w_out_hbm,
    w_gate_hbm,
    w_up_hbm,
    w_down_hbm,
    mixer_ref,
    expert_ref,
    value,
    gate,
    w_out,
    w_gate,
    w_up,
    w_down,
    load_sem,
    normed,
    slots,
    near_slots,
    onehots,
    arrived,
    near_send,
    near_recv,
    fn_send,
    fn_recv,
    a2a_send,
    a2a_recv,
    fx_send,
    fx_recv,
    fp_send,
    fp_recv,
    fq_send,
    fq_recv,
    gated,
    halo_in,
    halo_send,
    halo_recv,
    padded,
    conv,
    stat_out,
    stat_in,
    stat_send,
    stat_recv,
    act,
    mix_out,
    mix_own,
    mix_in,
    mix_send,
    mix_recv,
    mix_x_out,
    mix_x_in,
    mix_x_send,
    mix_x_recv,
    rs_out,
    rs_own,
    rs_in,
    rs_send,
    rs_recv,
    rx_out,
    rx_in,
    rx_send,
    rx_recv,
    answer,
    returned,
    ret_send,
    ret_recv,
    total,
):
    me = lax.axis_index("ep")
    mine = lax.axis_index("tp")
    core = lax.rem(mine, 2)
    chip = mine // 2
    partner = chip * 2 + 1 - core
    chips = tp // 2
    groups = n // group
    rows = group * cap
    tokens, width = moe_ref.shape
    quarter = width // tp
    length, chan = value.shape
    halo = halo_in.shape[0]
    own_rows = length // tp

    def toward(k):
        return lax.rem(me // 2 + k // 2, n // 2) * 2 + lax.rem(me + k, 2)

    def source(k):
        return lax.rem(me // 2 + n // 2 - k // 2, n // 2) * 2 + lax.rem(me + k, 2)

    def block(k):
        return pl.ds(pl.multiple_of(k * cap, cap), cap)

    def columns_of(part):
        return pl.ds(pl.multiple_of(part * quarter, 128), quarter)

    def across(j):
        there = lax.rem(chip + j, chips)
        here = lax.rem(chip + chips - j, chips)
        return there * 2 + core, here * 2 + core

    barrier = pltpu.get_barrier_semaphore()

    def greet_ep(k, _):
        pl.semaphore_signal(
            barrier, inc=1, device_id={"ep": lax.rem(me + k, n)}, device_id_type=MESH
        )
        return 0

    lax.fori_loop(1, n, greet_ep, 0)
    for j in range(1, tp):
        pl.semaphore_signal(
            barrier, inc=1, device_id={"tp": lax.rem(mine + j, tp)}, device_id_type=MESH
        )

    loads = [
        pltpu.make_async_copy(src, dst, load_sem.at[i])
        for i, (src, dst) in enumerate(
            [
                (value_hbm, value),
                (gate_hbm, gate),
                (w_out_hbm, w_out),
                (w_gate_hbm.at[0], w_gate),
                (w_up_hbm.at[0], w_up),
                (w_down_hbm.at[0], w_down),
            ]
        )
    ]
    for load in loads:
        load.start()

    everything = moe_ref[...].astype(f32)
    inverse = lax.rsqrt(jnp.sum(everything * everything, axis=1, keepdims=True) / width + eps_rms)
    normed[...] = (everything * inverse * moe_gain_ref[...]).astype(bf16)
    row = lax.broadcasted_iota(jnp.int32, (tokens, tokens), 0)
    col = lax.broadcasted_iota(jnp.int32, (tokens, tokens), 1)
    below = (col < row).astype(f32).astype(bf16)
    above = (row < col).astype(f32).astype(bf16)

    def a2a_copy(k):
        return pltpu.make_async_remote_copy(
            src_ref=slots.at[block(k)],
            dst_ref=arrived.at[mine, block(k)],
            send_sem=a2a_send.at[k],
            recv_sem=a2a_recv.at[k],
            device_id={"ep": toward(k)},
            device_id_type=MESH,
        )

    def near_copy(xx):
        return pltpu.make_async_remote_copy(
            src_ref=near_slots.at[xx],
            dst_ref=arrived.at[xx * 2 + core, pl.ds(cap, cap)],
            send_sem=near_send.at[xx],
            recv_sem=near_recv.at[xx],
            device_id={"ep": toward(1)},
            device_id_type=MESH,
        )

    def slot_picks(k):
        expert = toward(k)
        member = jnp.maximum(
            (ids_t_ref[0:1, :] == expert).astype(f32), (ids_t_ref[1:2, :] == expert).astype(f32)
        )
        member = jnp.broadcast_to(member, (cap, tokens))
        place = jnp.dot(member.astype(bf16), above, preferred_element_type=f32)
        slot = lax.broadcasted_iota(jnp.int32, (cap, tokens), 0).astype(f32)
        return jnp.where(place == slot, member, 0.0).astype(bf16)

    def picked(pick, part):
        return jnp.dot(
            pick, normed[:, columns_of(part)], preferred_element_type=f32
        ).astype(bf16)

    pl.semaphore_wait(barrier, n - 1 + tp - 1)

    def dispatch(k, _):
        slots[block(k), :] = picked(slot_picks(k), mine)
        a2a_copy(k).start()
        return 0

    lax.fori_loop(2, n, dispatch, 0)
    pick = slot_picks(1)
    for xx in range(chips):
        near_slots[xx] = picked(pick, xx * 2 + core)
        near_copy(xx).start()

    loads[0].wait()
    loads[1].wait()
    gated_now = (value[...].astype(f32) * jax.nn.sigmoid(gate[...].astype(f32))).astype(bf16)
    gated[...] = gated_now
    halo_copy = pltpu.make_async_remote_copy(
        src_ref=gated.at[pl.ds(length - halo, halo)],
        dst_ref=halo_in,
        send_sem=halo_send,
        recv_sem=halo_recv,
        device_id={"ep": lax.rem(me + 1, n)},
        device_id_type=MESH,
    )
    halo_copy.start()
    padded[pl.ds(halo, length), :] = gated_now.astype(f32)

    pick = slot_picks(0)
    for part in range(tp):
        arrived[part, 0:cap, :] = picked(pick, part)

    def fx_copy(k, j):
        to, _ = across(j)
        return pltpu.make_async_remote_copy(
            src_ref=arrived.at[mine, block(k)],
            dst_ref=arrived.at[mine, block(k)],
            send_sem=fx_send.at[k, j - 1],
            recv_sem=fx_recv.at[k, j - 1],
            device_id={"tp": to},
            device_id_type=MESH,
        )

    def fp_copy(k):
        return pltpu.make_async_remote_copy(
            src_ref=arrived.at[mine, block(k)],
            dst_ref=arrived.at[mine, block(k)],
            send_sem=fp_send.at[k],
            recv_sem=fp_recv.at[k],
            device_id={"tp": partner},
            device_id_type=MESH,
        )

    def fq_copy(k, j):
        _, origin = across(j)
        return pltpu.make_async_remote_copy(
            src_ref=arrived.at[origin, block(k)],
            dst_ref=arrived.at[origin, block(k)],
            send_sem=fq_send.at[k, j - 1],
            recv_sem=fq_recv.at[k, j - 1],
            device_id={"tp": partner},
            device_id_type=MESH,
        )

    def fn_copy(xx):
        return pltpu.make_async_remote_copy(
            src_ref=arrived.at[xx * 2 + core, pl.ds(cap, cap)],
            dst_ref=arrived.at[xx * 2 + core, pl.ds(cap, cap)],
            send_sem=fn_send.at[xx],
            recv_sem=fn_recv.at[xx],
            device_id={"tp": partner},
            device_id_type=MESH,
        )

    def over_group(g, do, first=2):
        def one(k, _):
            @pl.when(k >= first)
            def _():
                do(k)

            return 0

        lax.fori_loop(g * group, (g + 1) * group, one, 0)

    def forward_first(g):
        def one(k):
            a2a_copy(k).wait_recv()
            for j in range(1, chips):
                fx_copy(k, j).start()
            fp_copy(k).start()

        over_group(g, one)

    def forward_second(g):
        def one(k):
            for j in range(1, chips):
                fx_copy(k, j).wait_recv()
                fq_copy(k, j).start()

        over_group(g, one)

    def forward_near():
        for xx in range(chips):
            near_copy(xx).wait_recv()
            fn_copy(xx).start()

    halo_copy.wait_recv()
    padded[pl.ds(0, halo), :] = jnp.where(me == 0, 0.0, halo_in[...].astype(f32))
    step_rows = 64
    window = step_rows + halo

    for lane in range(0, chan, 128):

        def conv_step(i, _):
            base = pl.multiple_of(i * step_rows, step_rows)
            rows_in = padded[pl.ds(base, window), lane : lane + 128]
            result = jnp.zeros((step_rows, 128), f32)
            for shift in range(8):
                turned = rows_in if shift == 0 else pltpu.roll(rows_in, window - shift, 0)
                for tap in range(reach):
                    offset = halo - tap
                    if offset % 8 == shift:
                        begin = offset - shift
                        result = (
                            result
                            + taps_ref[tap : tap + 1, lane : lane + 128]
                            * turned[begin : begin + step_rows]
                        )
            conv[pl.ds(base, step_rows), lane : lane + 128] = result
            return 0

        lax.fori_loop(0, length // step_rows, conv_step, 0)

    convolved = conv[...]
    sums = jnp.sum(convolved, axis=1, keepdims=True)
    squares = jnp.sum(convolved * convolved, axis=1, keepdims=True)
    lanes = lax.broadcasted_iota(jnp.int32, (length, 128), 1)
    packed = jnp.where(lanes == 0, sums, jnp.where(lanes == 1, squares, 0.0))
    stat_out[...] = jnp.transpose(packed)[0:8]

    def stat_copy(j):
        return pltpu.make_async_remote_copy(
            src_ref=stat_out,
            dst_ref=stat_in.at[j - 1],
            send_sem=stat_send.at[j - 1],
            recv_sem=stat_recv.at[j - 1],
            device_id={"tp": lax.rem(mine + j, tp)},
            device_id_type=MESH,
        )

    for j in range(1, tp):
        stat_copy(j).start()

    forward_near()
    forward_first(0)
    if groups > 1:
        forward_first(1)
    forward_second(0)

    stats = stat_out[...]
    for j in range(1, tp):
        stat_copy(j).wait_recv()
        stats = stats + stat_in[j - 1]
    stats = jnp.concatenate([stats, jnp.zeros((120, length), f32)], axis=0)
    columns = jnp.transpose(stats)
    mean = columns[:, 0:1] / (chan * tp)
    variance = columns[:, 1:2] / (chan * tp) - mean * mean
    scaled = (conv[...] - mean) * lax.rsqrt(variance + eps_norm) * ln_gain_ref[...]
    act[...] = jax.nn.silu(scaled).astype(bf16)

    def mix_copy(xx):
        return pltpu.make_async_remote_copy(
            src_ref=mix_out.at[xx],
            dst_ref=mix_in.at[xx],
            send_sem=mix_send.at[xx],
            recv_sem=mix_recv.at[xx],
            device_id={"tp": partner},
            device_id_type=MESH,
        )

    def mix_part(owner):
        begin = pl.multiple_of(owner * own_rows, own_rows)
        return jnp.dot(act[pl.ds(begin, own_rows), :], w_out[...], preferred_element_type=f32)

    loads[2].wait()

    def mix_first(xx, _):
        mix_out[xx] = mix_part(xx * 2 + 1 - core).astype(bf16)
        mix_copy(xx).start()
        return 0

    def mix_second(xx, _):
        mix_own[xx] = mix_part(xx * 2 + core).astype(bf16)
        return 0

    lax.fori_loop(0, chips, mix_first, 0)
    lax.fori_loop(0, chips, mix_second, 0)

    half = own_rows // 2

    def mix_x_copy(j, part):
        to, _ = across(j)
        span = pl.ds(part * half, half)
        return pltpu.make_async_remote_copy(
            src_ref=mix_x_out.at[j - 1, span],
            dst_ref=mix_x_in.at[j - 1, span],
            send_sem=mix_x_send.at[j - 1, part],
            recv_sem=mix_x_recv.at[j - 1, part],
            device_id={"tp": to},
            device_id_type=MESH,
        )

    def mix_stage():
        for xx in range(chips):
            mix_copy(xx).wait_recv()
        for j in range(1, chips):
            there = lax.rem(chip + j, chips)
            mix_x_out[j - 1] = (mix_own[there].astype(f32) + mix_in[there].astype(f32)).astype(
                bf16
            )
    loads[3].wait()
    loads[4].wait()
    loads[5].wait()

    def rs_copy(g, xx):
        return pltpu.make_async_remote_copy(
            src_ref=rs_out.at[g, xx],
            dst_ref=rs_in.at[g, xx],
            send_sem=rs_send.at[g, xx],
            recv_sem=rs_recv.at[g, xx],
            device_id={"tp": partner},
            device_id_type=MESH,
        )

    def rx_copy(k, j):
        to, _ = across(j)
        return pltpu.make_async_remote_copy(
            src_ref=rx_out.at[j - 1, block(k)],
            dst_ref=rx_in.at[j - 1, block(k)],
            send_sem=rx_send.at[k, j - 1],
            recv_sem=rx_recv.at[k, j - 1],
            device_id={"tp": to},
            device_id_type=MESH,
        )

    def ret_copy(k):
        return pltpu.make_async_remote_copy(
            src_ref=answer.at[block(k)],
            dst_ref=returned.at[block(k)],
            send_sem=ret_send.at[k],
            recv_sem=ret_recv.at[k],
            device_id={"ep": source(k)},
            device_id_type=MESH,
        )

    def expert_step(g):
        @pl.when(g == 0)
        def _():
            for xx in range(chips):
                fn_copy(xx).wait_recv()

        def one(k):
            fp_copy(k).wait_recv()
            for j in range(1, chips):
                fq_copy(k, j).wait_recv()

        over_group(g, one)
        span = pl.ds(pl.multiple_of(g * rows, rows), rows)
        x = jnp.concatenate([arrived[part, span] for part in range(tp)], axis=1)
        gate_act = jnp.dot(x, w_gate[...], preferred_element_type=f32)
        up_act = jnp.dot(x, w_up[...], preferred_element_type=f32)
        hidden = (jax.nn.silu(gate_act) * up_act).astype(bf16)
        for xx in range(chips):
            begin = pl.multiple_of((xx * 2 + 1 - core) * quarter, 128)
            rs_out[g, xx] = jnp.dot(
                hidden, w_down[:, pl.ds(begin, quarter)], preferred_element_type=f32
            ).astype(bf16)
            rs_copy(g, xx).start()
        for xx in range(chips):
            begin = pl.multiple_of((xx * 2 + core) * quarter, 128)
            rs_own[g, xx] = jnp.dot(
                hidden, w_down[:, pl.ds(begin, quarter)], preferred_element_type=f32
            ).astype(bf16)

    def sum_step(g):
        for xx in range(chips):
            rs_copy(g, xx).wait_recv()
        span = pl.ds(pl.multiple_of(g * rows, rows), rows)
        for j in range(1, chips):
            there = lax.rem(chip + j, chips)
            rx_out[j - 1, span] = (
                rs_own[g, there].astype(f32) + rs_in[g, there].astype(f32)
            ).astype(bf16)

        def one(k):
            for j in range(1, chips):
                rx_copy(k, j).start()

        over_group(g, one, 0)

    def return_step(g):
        def one(k):
            inner = pl.ds(pl.multiple_of((k - g * group) * cap, cap), cap)
            result = rs_own[g, chip, inner].astype(f32) + rs_in[g, chip, inner].astype(f32)
            for j in range(1, chips):
                rx_copy(k, j).wait_recv()
                result = result + rx_in[j - 1, block(k)].astype(f32)
            answer[block(k), :] = result.astype(bf16)

            @pl.when(k > 0)
            def _():
                ret_copy(k).start()

        over_group(g, one, 0)

    total[...] = jnp.zeros_like(total)

    def combine_step(g):
        def take(k, _):
            @pl.when(k > 0)
            def _():
                ret_copy(k).wait_recv()

            expert = toward(k)
            weight = jnp.where(ids_ref[:, 0:1] == expert, route_ref[:, 0:1], 0.0) + jnp.where(
                ids_ref[:, 1:2] == expert, route_ref[:, 1:2], 0.0
            )
            answers = returned[block(k), :]
            total[...] += weight * jnp.dot(onehots[k], answers, preferred_element_type=f32)
            return 0

        lax.fori_loop(g * group, (g + 1) * group, take, 0)

    def place_of(k, _):
        expert = toward(k)
        member = jnp.maximum(
            (ids_ref[:, 0:1] == expert).astype(f32), (ids_ref[:, 1:2] == expert).astype(f32)
        )
        member = jnp.broadcast_to(member, (tokens, cap))
        place = jnp.dot(below, member.astype(bf16), preferred_element_type=f32)
        slot = lax.broadcasted_iota(jnp.int32, (tokens, cap), 1).astype(f32)
        onehots[k] = jnp.where(place == slot, member, 0.0).astype(bf16)
        return 0

    def step(g, _):
        @pl.when(g < groups)
        def _():
            expert_step(g)

        @pl.when(g < groups)
        def _():
            sum_step(g)

        @pl.when(g + 1 < groups)
        def _():
            forward_second(g + 1)

        @pl.when(g == groups)
        def _():
            lax.fori_loop(0, n, place_of, 0)

        @pl.when((g >= 1) & (g < groups + 1))
        def _():
            return_step(g - 1)

        @pl.when(g == 0)
        def _():
            mix_stage()

        @pl.when(g + 2 < groups)
        def _():
            forward_first(g + 2)

        @pl.when(g == groups - 1)
        def _():
            for j in range(1, chips):
                mix_x_copy(j, 0).start()
                mix_x_copy(j, 1).start()

        return 0

    lax.fori_loop(0, groups + 1, step, 0)
    returned[0:cap, :] = answer[0:cap, :]

    def combine(g, _):
        combine_step(g)
        return 0

    lax.fori_loop(0, groups, combine, 0)
    expert_ref[...] = total[...].astype(bf16)

    mixed = mix_own[chip].astype(f32) + mix_in[chip].astype(f32)
    for j in range(1, chips):
        mix_x_copy(j, 0).wait_recv()
        mix_x_copy(j, 1).wait_recv()
        mixed = mixed + mix_x_in[j - 1].astype(f32)
    mixer_ref[...] = mixed.astype(bf16)

    ret_copy(1).wait_send()

    def left(k, _):
        a2a_copy(k).wait_send()
        ret_copy(k).wait_send()
        fp_copy(k).wait_send()
        for j in range(1, chips):
            fx_copy(k, j).wait_send()
            fq_copy(k, j).wait_send()
        return 0

    lax.fori_loop(2, n, left, 0)

    def left_x(k, _):
        for j in range(1, chips):
            rx_copy(k, j).wait_send()
        return 0

    lax.fori_loop(0, n, left_x, 0)
    halo_copy.wait_send()
    for j in range(1, tp):
        stat_copy(j).wait_send()
    for xx in range(chips):
        mix_copy(xx).wait_send()
        near_copy(xx).wait_send()
        fn_copy(xx).wait_send()
    for j in range(1, chips):
        mix_x_copy(j, 0).wait_send()
        mix_x_copy(j, 1).wait_send()

    def left_group(g, _):
        for xx in range(chips):
            rs_copy(g, xx).wait_send()
        return 0

    lax.fori_loop(0, groups, left_group, 0)


def on_device(
    glu_value,
    glu_gate,
    conv_kernel,
    ln_gain,
    out_weight,
    moe_input,
    moe_gain,
    gate_weight,
    up_weight,
    down_weight,
    expert_ids,
    route_weight,
):
    n = lax.axis_size("ep")
    tp = lax.axis_size("tp")
    chips = tp // 2
    length, chan = glu_value.shape
    reach = conv_kernel.shape[0]
    halo = -(-(reach - 1) // 16) * 16
    tokens, width = moe_input.shape
    hidden = gate_weight.shape[2]
    cap = 4 * max(1, tokens // n)
    group = max(1, min(n, 256 // cap))
    groups = n // group
    rows = group * cap
    quarter = width // tp
    own_rows = length // tp
    vmem = pl.BlockSpec(memory_space=pltpu.VMEM)
    hbm = pl.BlockSpec(memory_space=pl.ANY)
    dma = pltpu.SemaphoreType.DMA
    V = pltpu.VMEM
    others = max(1, chips - 1)
    return pl.pallas_call(
        functools.partial(kernel, n, tp, cap, group, reach),
        out_shape=(
            jax.ShapeDtypeStruct((own_rows, out_weight.shape[1]), bf16),
            jax.ShapeDtypeStruct((tokens, quarter), bf16),
        ),
        in_specs=[vmem] * 7 + [hbm] * 6,
        out_specs=(vmem, vmem),
        scratch_shapes=[
            V((length, chan), bf16),
            V((length, chan), bf16),
            V(out_weight.shape, bf16),
            V((width, hidden), bf16),
            V((width, hidden), bf16),
            V((hidden, width), bf16),
            dma((6,)),
            V((tokens, width), bf16),
            V((n * cap, quarter), bf16),
            V((chips, cap, quarter), bf16),
            V((n, tokens, cap), bf16),
            V((tp, n * cap, quarter), bf16),
            dma((chips,)),
            dma((chips,)),
            dma((chips,)),
            dma((chips,)),
            dma((n,)),
            dma((n,)),
            dma((n, others)),
            dma((n, others)),
            dma((n,)),
            dma((n,)),
            dma((n, others)),
            dma((n, others)),
            V((length, chan), bf16),
            V((halo, chan), bf16),
            dma,
            dma,
            V((length + halo, chan), f32),
            V((length, chan), f32),
            V((8, length), f32),
            V((tp - 1, 8, length), f32),
            dma((tp - 1,)),
            dma((tp - 1,)),
            V((length, chan), bf16),
            V((chips, own_rows, out_weight.shape[1]), bf16),
            V((chips, own_rows, out_weight.shape[1]), bf16),
            V((chips, own_rows, out_weight.shape[1]), bf16),
            dma((chips,)),
            dma((chips,)),
            V((others, own_rows, out_weight.shape[1]), bf16),
            V((others, own_rows, out_weight.shape[1]), bf16),
            dma((others, 2)),
            dma((others, 2)),
            V((groups, chips, rows, quarter), bf16),
            V((groups, chips, rows, quarter), bf16),
            V((groups, chips, rows, quarter), bf16),
            dma((groups, chips)),
            dma((groups, chips)),
            V((others, n * cap, quarter), bf16),
            V((others, n * cap, quarter), bf16),
            dma((n, others)),
            dma((n, others)),
            V((n * cap, quarter), bf16),
            V((n * cap, quarter), bf16),
            dma((n,)),
            dma((n,)),
            V((tokens, quarter), f32),
        ],
        compiler_params=pltpu.CompilerParams(
            collective_id=0, has_side_effects=True, vmem_limit_bytes=60 * 1024 * 1024
        ),
        name="block",
    )(
        moe_input,
        moe_gain.reshape(1, -1),
        expert_ids,
        expert_ids.T,
        route_weight,
        conv_kernel,
        ln_gain.reshape(1, -1),
        glu_value,
        glu_gate,
        out_weight,
        gate_weight,
        up_weight,
        down_weight,
    )


def solution(mesh):
    in_specs = (
        P("ep", "tp"),
        P("ep", "tp"),
        P(None, "tp"),
        P("tp"),
        P("tp", None),
        P("ep", None),
        P(),
        P("ep", None, "tp"),
        P("ep", None, "tp"),
        P("ep", "tp", None),
        P("ep", None),
        P("ep", None),
    )
    out_specs = (P(("ep", "tp"), None), P("ep", "tp"))
    return jax.shard_map(
        on_device, mesh=mesh, in_specs=in_specs, out_specs=out_specs, check_vma=False
    )
```
